32 devices in a mesh: kv: 8 (over z, x), tp: 4 (over y, core).
Axes of the slice: x: 2, y: 2, z: 4, core: 2. Of those that a mesh axis runs over, the one named last changes fastest.
Arguments:
- tokens: bfloat16 [288, 4096], P(None, 'kv'), may hold values from -40 to 40
- norm_gain: float32 [4096], P('kv'), may hold values from 0.1 to 1.9
- query_weight: bfloat16 [4096, 2048], P('kv', 'tp'), may hold values from -0.09375 to 0.09375
- key_weight: bfloat16 [4096, 2048], P('kv', 'tp'), may hold values from -0.09375 to 0.09375
- value_weight: bfloat16 [4096, 2048], P('kv', 'tp'), may hold values from -0.09375 to 0.09375
- gate_weight: bfloat16 [4096, 32], replicated, may hold values from -0.09375 to 0.09375
- gate_bias: float32 [32], replicated, may hold values from -0.5 to 3
- out_weight: bfloat16 [2048, 4096], P('tp', 'kv'), may hold values from -0.125 to 0.125
- cache_keys: bfloat16 [12, 3072, 2048], P(None, 'kv', 'tp'), may hold values from -1000 to 1000
- cache_values: bfloat16 [12, 3072, 2048], P(None, 'kv', 'tp'), may hold values from -6 to 6
- cache_decay: float32 [12, 32, 3072], P(None, 'tp', 'kv'), may hold values from -3072 to 0, as said below
- lengths: int32 [12], replicated, may hold values from 1537 to 3072
- parents: int32 [12, 24], replicated, may hold values from 0 to 23, as said below
Outputs:
- mixed: bfloat16 [288, 4096], P('tp', 'kv')
The draws below stay inside these ranges and needn't reach their ends.
Inputs may be any that keep to these rules, and one draw needn't show every extreme that they name: `cache_decay`: zero at and beyond lengths of the sequence. parents[s, 0] = 0 and parents[s, n] < n for n > 0.
All inputs are finite; a program needn't handle non-finite values.
Results may differ from the reference program's by a relative error of at most 0.014.
The reference program's roundings to bfloat16 on the way count: a program that leaves them out, or rounds other values in their place, can miss the bound.
Values may be sent and summed in bfloat16 or wider, within the bound.
A program may use at most 64 MiB of HBM per device.

```python
import jax
import jax.numpy as jnp
from jax import lax

D = 4096
ATTENTION_HEADS = 32
HEAD_DIM = 64
SEQUENCE_COUNT = 12
PROPS = 24
POS_DEV = 384
ROWS = 288
CACHE_LENGTH = 3072
GROUP_HEADS = 8
N_KV = 8
N_TP = 4


def length_draw(key):
    drawn = jax.random.randint(jax.random.fold_in(key, 11), (SEQUENCE_COUNT,), CACHE_LENGTH // 2 + 1, CACHE_LENGTH + 1).astype(jnp.int32)
    order = jax.random.permutation(jax.random.fold_in(key, 12), SEQUENCE_COUNT)
    drawn = jnp.where(order == 0, CACHE_LENGTH, drawn)
    return drawn.astype(jnp.int32)


def draw_lengths(key, part):
    return length_draw(key)


def draw_parents(key, part):
    nodes = jnp.arange(PROPS, dtype=jnp.int32)
    lowest = jnp.maximum(nodes - 4, 0)
    spread = jnp.maximum(nodes - lowest, 1)
    raw = jax.random.randint(jax.random.fold_in(key, 3), (SEQUENCE_COUNT, PROPS), 0, 1 << 20)
    picked = lowest[None, :] + raw % spread[None, :]
    return jnp.where(nodes[None, :] > 0, picked, 0).astype(jnp.int32)


def draw_tokens(key, part):
    column = jnp.arange(D, dtype=jnp.float32) / D
    jitter = jnp.exp(jax.random.uniform(jax.random.fold_in(key, 1), (D,), jnp.float32, -0.5, 0.5))
    ramp = jnp.exp(jnp.log(0.4) + jnp.log(9.0) * column)
    base = jnp.clip(jax.random.normal(jax.random.fold_in(key, 2), (ROWS, D), jnp.float32), -6.0, 6.0)
    values = base * ramp[None, :] * jitter[None, :]
    return values.astype(jnp.bfloat16)


def draw_cache_keys(key, part):
    shape = (SEQUENCE_COUNT, CACHE_LENGTH, ATTENTION_HEADS * HEAD_DIM)
    base = jnp.clip(jax.random.normal(jax.random.fold_in(key, 1), shape, jnp.float32), -6.0, 6.0)
    return base.astype(jnp.bfloat16)


def draw_cache_decay(key, part):
    lengths = length_draw(key)
    order = jax.random.permutation(jax.random.fold_in(key, 21), ATTENTION_HEADS)
    slow_decay = order < ATTENTION_HEADS // 2
    slow_rate = 0.6 / CACHE_LENGTH * jnp.exp(jax.random.uniform(jax.random.fold_in(key, 22), (ATTENTION_HEADS,), jnp.float32, -0.7, 0.7))
    fast_rate = jnp.exp(-jax.random.uniform(jax.random.fold_in(key, 23), (ATTENTION_HEADS,), jnp.float32, jnp.log(30.0), jnp.log(100.0)))
    rate = jnp.where(slow_decay, slow_rate, fast_rate)
    rough = jnp.exp(jax.random.uniform(jax.random.fold_in(key, 24), (SEQUENCE_COUNT, ATTENTION_HEADS, CACHE_LENGTH), jnp.float32, -0.7, 0.7))
    blocks = jnp.exp(jax.random.uniform(jax.random.fold_in(key, 25), (SEQUENCE_COUNT, ATTENTION_HEADS, CACHE_LENGTH // POS_DEV), jnp.float32, -0.7, 0.7))
    blocks = jnp.repeat(blocks, POS_DEV, axis=2)
    forget_gates = -rate[None, :, None] * rough * blocks
    window_count = jax.random.randint(jax.random.fold_in(key, 26), (SEQUENCE_COUNT, ATTENTION_HEADS, CACHE_LENGTH), 0, CACHE_LENGTH) < 3
    window_length = jax.random.uniform(jax.random.fold_in(key, 27), (SEQUENCE_COUNT, ATTENTION_HEADS, CACHE_LENGTH), jnp.float32, 0.22, 0.69)
    forget_gates = forget_gates - jnp.where(window_count & slow_decay[None, :, None], window_length, 0.0)
    position = jnp.arange(CACHE_LENGTH, dtype=jnp.int32)
    live = position[None, None, :] < lengths[:, None, None]
    forget_gates = jnp.where(live, forget_gates, 0.0)
    running = jnp.cumsum(forget_gates, axis=2)
    return jnp.where(live, running[:, :, -1:] - running, 0.0)


def shard_levels(rng, shape, pieces, least, largest):
    factor_of, own = 1.0, jax.random.fold_in(rng, 6)
    for dim, blocks in pieces:
        steps = jnp.exp(jax.random.uniform(jax.random.fold_in(own, dim), (blocks,), jnp.float32, least / len(pieces), largest / len(pieces)))
        factor_of = factor_of * jnp.repeat(steps, shape[dim] // blocks).reshape([-1 if axis == dim else 1 for axis in range(len(shape))])
    return factor_of


def noise(rng, shape, width, bound, cuts=(), held_as=jnp.bfloat16):
    factor_of = shard_levels(rng, shape, cuts, -0.22, 0.18) if cuts else 1.0
    values = jax.random.normal(rng, shape, jnp.float32) * width * factor_of
    return jnp.minimum(jnp.maximum(values, -bound), bound).astype(held_as)


def setup_inputs(seed: int = 0) -> dict:
    streams_of = jax.random.split(jax.random.key(seed), 14)
    tokens = draw_tokens(jax.random.fold_in(streams_of[13], 71), 0)
    norm_gain = jnp.clip(1.0 + 0.18 * jax.random.normal(streams_of[1], (D,), jnp.float32), 0.1, 1.9)
    query_weight = noise(streams_of[2], (D, ATTENTION_HEADS * HEAD_DIM), D ** -0.5, 0.09375, ((0, 8), (1, 4)))
    key_weight = noise(streams_of[3], (D, ATTENTION_HEADS * HEAD_DIM), D ** -0.5, 0.09375, ((0, 8), (1, 4)))
    value_weight = noise(streams_of[4], (D, ATTENTION_HEADS * HEAD_DIM), D ** -0.5, 0.09375, ((0, 8), (1, 4)))
    gate_weight = noise(streams_of[5], (D, ATTENTION_HEADS), D ** -0.5, 0.09375)
    gate_bias = jnp.clip(jax.random.uniform(streams_of[6], (ATTENTION_HEADS,), jnp.float32, -0.5, 3.0), -0.5, 3.0)
    out_weight = noise(streams_of[7], (ATTENTION_HEADS * HEAD_DIM, D), (ATTENTION_HEADS * HEAD_DIM) ** -0.5, 0.125, ((0, 4), (1, 8)))
    cache_keys = draw_cache_keys(jax.random.fold_in(streams_of[13], 71), 0)
    cache_values = noise(streams_of[9], (SEQUENCE_COUNT, CACHE_LENGTH, ATTENTION_HEADS * HEAD_DIM), 1.0, 6.0, ((1, 8), (2, 4)))
    cache_decay = draw_cache_decay(jax.random.fold_in(streams_of[13], 71), 0)
    lengths = draw_lengths(jax.random.fold_in(streams_of[13], 71), 0)
    parents = draw_parents(jax.random.fold_in(streams_of[13], 71), 0)
    return dict(tokens=tokens, norm_gain=norm_gain, query_weight=query_weight, key_weight=key_weight, value_weight=value_weight, gate_weight=gate_weight, gate_bias=gate_bias, out_weight=out_weight, cache_keys=cache_keys, cache_values=cache_values, cache_decay=cache_decay, lengths=lengths, parents=parents)


def ancestry_of(parents):
    count = parents.shape[1]
    nodes = jnp.arange(count, dtype=jnp.int32)
    link = (parents[:, :, None] == nodes[None, None, :]).astype(jnp.float32)
    link = jnp.maximum(link, jnp.eye(count, dtype=jnp.float32)[None])
    for _ in range(count.bit_length()):
        link = jnp.minimum(jnp.einsum('snm,smk->snk', link, link, precision=lax.Precision.HIGHEST), 1.0)
    return link

def reference(tokens, norm_gain, query_weight, key_weight, value_weight, gate_weight, gate_bias, out_weight, cache_keys, cache_values, cache_decay, lengths, parents):
    scale = HEAD_DIM ** (-0.5)
    xf = tokens.astype(jnp.float32)
    inverse = lax.rsqrt(lax.optimization_barrier(jnp.mean(xf * xf, axis=1, keepdims=True)) + 1e-06)
    normed = (xf * norm_gain).astype(jnp.bfloat16)

    def project(weight):
        return (inverse * jnp.dot(normed, weight, preferred_element_type=jnp.float32)).astype(jnp.bfloat16)
    queries = project(query_weight).astype(jnp.float32).reshape(SEQUENCE_COUNT, PROPS, ATTENTION_HEADS, HEAD_DIM)
    new_keys = project(key_weight).astype(jnp.float32).reshape(SEQUENCE_COUNT, PROPS, ATTENTION_HEADS, HEAD_DIM)
    new_values = project(value_weight).astype(jnp.float32).reshape(SEQUENCE_COUNT, PROPS, ATTENTION_HEADS, HEAD_DIM)
    log_gates = jax.nn.log_sigmoid(inverse * jnp.dot(normed, gate_weight, preferred_element_type=jnp.float32) + gate_bias)
    log_gates = log_gates.reshape(SEQUENCE_COUNT, PROPS, ATTENTION_HEADS)
    ancestry = ancestry_of(parents)
    path = jnp.einsum('snk,skh->snh', ancestry, log_gates, precision=lax.Precision.HIGHEST)

    def cache_block(block):
        start = (block * POS_DEV).astype(jnp.int32)
        keys_blk = lax.dynamic_slice_in_dim(cache_keys, start, POS_DEV, 1).astype(jnp.float32).reshape(SEQUENCE_COUNT, POS_DEV, ATTENTION_HEADS, HEAD_DIM)
        vals_blk = lax.dynamic_slice_in_dim(cache_values, start, POS_DEV, 1).astype(jnp.float32).reshape(SEQUENCE_COUNT, POS_DEV, ATTENTION_HEADS, HEAD_DIM)
        decay_blk = lax.dynamic_slice_in_dim(cache_decay, start, POS_DEV, 2)
        scores = jnp.einsum('snhd,sjhd->snhj', queries, keys_blk) * scale
        scores = scores + path[..., None] + decay_blk[:, None, :, :]
        position = start + jnp.arange(POS_DEV, dtype=jnp.int32)
        live = (position[None, :] < lengths[:, None])[:, None, None, :]
        scores = jnp.where(live, scores, -1e+30)
        top = lax.optimization_barrier(jnp.max(scores, axis=-1))
        weights = jnp.where(live, jnp.exp(scores - top[..., None]), 0.0)
        total = lax.optimization_barrier(jnp.sum(weights, axis=-1))
        rounded = lax.optimization_barrier(weights.astype(jnp.bfloat16)).astype(jnp.float32)
        mix = jnp.einsum('snhj,sjhd->snhd', rounded, vals_blk)
        return (top, total, mix)
    tops, totals, mixes = lax.map(cache_block, jnp.arange(N_KV, dtype=jnp.int32))
    tree_scores = jnp.einsum('snhd,skhd->snhk', queries, new_keys) * scale
    tree_scores = tree_scores + path[..., None] - jnp.swapaxes(path, 1, 2)[:, None, :, :]
    tree_live = ancestry[:, :, None, :] > 0.5
    tree_scores = jnp.where(tree_live, tree_scores, -1e+30)
    tree_top = lax.optimization_barrier(jnp.max(tree_scores, axis=-1))
    tree_weights = jnp.where(tree_live, jnp.exp(tree_scores - tree_top[..., None]), 0.0)
    tree_total = lax.optimization_barrier(jnp.sum(tree_weights, axis=-1))
    tree_rounded = lax.optimization_barrier(tree_weights.astype(jnp.bfloat16)).astype(jnp.float32)
    tree_mix = jnp.einsum('snhk,skhd->snhd', tree_rounded, new_values)
    best = jnp.maximum(lax.optimization_barrier(jnp.max(tops, axis=0)), tree_top)
    factors = jnp.exp(tops - best[None])
    tree_factor = jnp.exp(tree_top - best)
    numer = lax.optimization_barrier(jnp.sum(factors[..., None] * mixes, axis=0)) + tree_factor[..., None] * tree_mix
    denom = lax.optimization_barrier(jnp.sum(factors * totals, axis=0)) + tree_factor * tree_total
    attended = (numer / denom[..., None]).reshape(ROWS, ATTENTION_HEADS * HEAD_DIM).astype(jnp.bfloat16)
    group = GROUP_HEADS * HEAD_DIM
    mixed = jnp.zeros((ROWS, D), jnp.float32)
    for index in range(N_TP):
        part = jnp.dot(attended[:, index * group:(index + 1) * group], out_weight[index * group:(index + 1) * group], preferred_element_type=jnp.float32)
        mixed = mixed + lax.optimization_barrier(part.astype(jnp.bfloat16)).astype(jnp.float32)
    return mixed.astype(jnp.bfloat16)
```

```python
import functools

import jax
import jax.numpy as jnp
from jax import lax
from jax.experimental import pallas as pl
from jax.experimental.pallas import tpu as pltpu
from jax.sharding import PartitionSpec as P

F32 = jnp.float32
BF16 = jnp.bfloat16
LANES = 128
LOW = -1e30
NT = (((1,), (1,)), ((), ()))
HIGH = lax.Precision.HIGHEST


def dot(a, b, precision=None):
    return jnp.dot(a, b, preferred_element_type=F32, precision=precision)


def dot_nt(a, b, precision=None):
    return lax.dot_general(a, b, NT, preferred_element_type=F32, precision=precision)


def fold(x):
    half = x.shape[1] // 2
    return jnp.concatenate([x[:, :half], x[:, half:]], axis=0)


def unfold(x):
    rows = x.shape[0] // 2
    x = x.astype(F32)
    return jnp.concatenate([x[:rows], x[rows:]], axis=1)


def kernel(
    n,
    n_tp,
    tokens,
    gain,
    query_w,
    key_w,
    value_w,
    gate_hbm,
    bias,
    out_hbm,
    keys_hbm,
    values_hbm,
    decay,
    lengths,
    parents,
    out,
    part,
    part_in,
    gate_w,
    out_w,
    keys,
    values,
    qbuf,
    mix,
    stat,
    mix_in,
    stat_in,
    att,
    anc,
    path_s,
    tmix,
    tstat,
    kvnew,
    terms,
    terms_in,
    par_pad,
    load_sem,
    cache_sem,
    a_send,
    a_recv,
    b_send,
    b_recv,
    c_send,
    c_recv,
    d_send,
    d_recv,
    e_send,
    e_recv,
):
    me = lax.axis_index("kv")
    tp = lax.axis_index("tp")
    rows, depth = tokens.shape
    seqs, props = parents.shape
    heads = decay.shape[1]
    pos_dev = keys.shape[1]
    width = query_w.shape[1]
    head_dim = width // heads
    scale = head_dim ** (-0.5)
    slots = part_in.shape[1]
    parity = lax.rem(tp, 2)
    left_over = seqs % n
    hp = heads * props

    barrier = pltpu.get_barrier_semaphore()
    for k in range(1, n):
        pl.semaphore_signal(barrier, inc=1, device_id={"kv": lax.rem(me + k, n)})
    for k in range(1, n_tp):
        pl.semaphore_signal(barrier, inc=1, device_id={"tp": lax.rem(tp + k, n_tp)})

    gate_load = pltpu.make_async_copy(
        gate_hbm.at[pl.ds(pl.multiple_of(me * depth, depth), depth), :], gate_w, load_sem.at[0]
    )
    gate_load.start()
    cache_loads = []
    for s in range(seqs):
        k_load = pltpu.make_async_copy(keys_hbm.at[s], keys.at[s], cache_sem.at[0, s])
        v_load = pltpu.make_async_copy(values_hbm.at[s], values.at[s], cache_sem.at[1, s])
        k_load.start()
        v_load.start()
        cache_loads.append((k_load, v_load))
    out_load = pltpu.make_async_copy(out_hbm, out_w, load_sem.at[1])
    out_load.start()

    def owner_of(s):
        if isinstance(s, int):
            place = s % n
            shift = parity * left_over if s // n == seqs // n else 0
        else:
            place = lax.rem(s, n)
            shift = jnp.where(lax.div(s, n) == seqs // n, parity * left_over, 0)
        return lax.rem(place + shift, n)

    def slot_seq(r):
        shift = parity * left_over if r == seqs // n else 0
        return r * n + lax.rem(me + 2 * n - shift, n)

    def for_slot(r, f):
        if (r + 1) * n <= seqs:
            f()
        else:
            pl.when(slot_seq(r) < seqs)(f)

    xf = tokens[...].astype(F32)
    squares = jnp.sum(xf * xf, axis=1, keepdims=True)
    normed = (xf * gain[...]).astype(BF16)
    sel_rows = lax.broadcasted_iota(jnp.int32, (bias.shape[1], LANES), 0)
    sel_cols = lax.broadcasted_iota(jnp.int32, (bias.shape[1], LANES), 1)
    select = ((sel_rows == sel_cols + tp * heads) & (sel_cols < heads)).astype(F32)
    for i, w in enumerate((query_w, key_w, value_w)):
        part[:, :, i * width : (i + 1) * width] = dot(normed, w[...]).reshape(seqs, props, width)
    gate_load.wait()
    gates_w = dot(gate_w[...], select.astype(BF16)).astype(BF16)
    gate_part = dot(normed, gates_w)
    lane = lax.broadcasted_iota(jnp.int32, (rows, LANES), 1)
    gate_part = jnp.where(lane == LANES // 2, squares, gate_part)
    part[:, :, 3 * width :] = gate_part.reshape(seqs, props, LANES)
    pl.semaphore_wait(barrier, n + n_tp - 2)

    def a_copy(s):
        d = owner_of(s)
        k = lax.rem(me - d + n, n)
        return d, pltpu.make_async_remote_copy(
            src_ref=part.at[s],
            dst_ref=part_in.at[jnp.maximum(k - 1, 0), s // n],
            send_sem=a_send.at[s],
            recv_sem=a_recv.at[jnp.maximum(k - 1, 0), s // n],
            device_id={"kv": d},
        )

    for s in range(seqs):
        d, copy = a_copy(s)
        pl.when(d != me)(copy.start)

    par_pad[...] = jnp.zeros(par_pad.shape, jnp.int32)
    par_pad[0:seqs, 0:props] = parents[...]
    r_i = lax.broadcasted_iota(jnp.int32, (LANES, LANES), 0)
    c_i = lax.broadcasted_iota(jnp.int32, (LANES, LANES), 1)
    eye = (r_i == c_i).astype(F32)
    bias_row = dot(jnp.broadcast_to(bias[...], (8, bias.shape[1])), select, HIGH)[0:1]

    def ancestry(r):
        s = slot_seq(r)
        row = par_pad[pl.ds(s, 1), :]
        link = jnp.maximum((row == r_i).astype(F32), eye).astype(BF16)
        for _ in range(props.bit_length()):
            link = jnp.minimum(dot(link, link), 1.0).astype(BF16)
        anc[r] = dot_nt(eye.astype(BF16), link)[:props]

    for r in range(slots):
        for_slot(r, functools.partial(ancestry, r))

    lane_p = lax.broadcasted_iota(jnp.int32, (props, LANES), 1)
    bd_row = lax.broadcasted_iota(jnp.int32, (heads, props, width), 0)
    bd_col = lax.broadcasted_iota(jnp.int32, (heads, props, width), 2)
    diag = (lax.div(bd_col, head_dim) == bd_row).reshape(hp, width)

    def spread(q):
        wide = jnp.broadcast_to(q[None], (heads, props, width)).reshape(hp, width)
        return jnp.where(diag, wide, 0.0).astype(BF16)

    def gather_diag(m):
        return jnp.sum(jnp.where(diag, m, 0.0).reshape(heads, props, width), axis=0)

    def to_lanes(col, first):
        acc = jnp.zeros((props, LANES), F32)
        for h in range(heads):
            acc = jnp.where(lane_p == h + first, col[h * props : (h + 1) * props], acc)
        return acc

    def b_copy(r, k, buf, send, recv):
        s = slot_seq(r)
        return pltpu.make_async_remote_copy(
            src_ref=buf.at[s],
            dst_ref=buf.at[s],
            send_sem=send.at[r, k - 1],
            recv_sem=recv.at[s],
            device_id={"kv": lax.rem(me + k, n)},
        )

    pad_rows = LANES - props

    def project(r):
        s = slot_seq(r)
        for k in range(1, n):
            pltpu.make_async_remote_copy(
                src_ref=part.at[0],
                dst_ref=part_in.at[k - 1, r],
                send_sem=a_send.at[0],
                recv_sem=a_recv.at[k - 1, r],
                device_id={"kv": lax.rem(me + k, n)},
            ).wait_recv()
        total = part[s]
        for k in range(1, n):
            total = total + part_in[k - 1, r]
        tail = total[:, 3 * width :]
        square = jnp.sum(jnp.where(lane_p == LANES // 2, tail, 0.0), axis=1, keepdims=True)
        inverse = lax.rsqrt(square / (depth * n) + 1e-06)
        q = inverse * total[:, :width]
        qbuf[s] = fold(q).astype(BF16)
        for k in range(1, n):
            b_copy(r, k, qbuf, b_send, b_recv).start()
        kvnew[r, 0, 0:props] = inverse * total[:, width : 2 * width]
        kvnew[r, 1, 0:props] = inverse * total[:, 2 * width : 3 * width]
        kvnew[r, :, props:] = jnp.zeros((2, pad_rows, width), F32)
        x = inverse * tail + bias_row
        log_gate = jnp.minimum(x, 0.0) - jnp.log1p(jnp.exp(-jnp.abs(x)))
        padded = jnp.concatenate([log_gate, jnp.zeros((pad_rows, LANES), F32)], axis=0)
        path_s[r] = dot(anc[r], padded, HIGH)

    for r in range(slots):
        for_slot(r, functools.partial(project, r))

    def tree(r):
        s = slot_seq(r)
        path = path_s[r]
        q = spread(unfold(qbuf[s]))
        head_of = lax.broadcasted_iota(jnp.int32, (heads, props, LANES), 0)
        lane_of = lax.broadcasted_iota(jnp.int32, (heads, props, LANES), 2)
        pick = (head_of == lane_of).reshape(hp, LANES)
        tiled = jnp.broadcast_to(path[None], (heads, props, LANES)).reshape(hp, LANES)
        own = jnp.sum(jnp.where(pick, tiled, 0.0), axis=1, keepdims=True)
        padded = jnp.concatenate([path, jnp.zeros((pad_rows, LANES), F32)], axis=0)
        other = dot_nt(pick.astype(F32), padded, HIGH)
        scores = dot_nt(q, kvnew[r, 0].astype(BF16)) * scale + own - other
        live = jnp.broadcast_to(anc[r][None], (heads, props, LANES)).reshape(hp, LANES) > 0.5
        scores = jnp.where(live, scores, LOW)
        top = jnp.max(scores, axis=1, keepdims=True)
        w = jnp.where(live, jnp.exp(scores - top), 0.0)
        total = jnp.sum(w, axis=1, keepdims=True)
        tmix[r] = gather_diag(dot(w.astype(BF16), kvnew[r, 1].astype(BF16)))
        tstat[r, 0] = to_lanes(top, 0)
        tstat[r, 1] = to_lanes(total, 0)

    for r in range(slots):
        for_slot(r, functools.partial(tree, r))

    position = lax.broadcasted_iota(jnp.int32, (hp, pos_dev), 1) + me * pos_dev

    def c_copy(s, which, src, dst):
        d = owner_of(s)
        k = jnp.maximum(lax.rem(me - d + n, n) - 1, 0)
        slot = s // n if isinstance(s, int) else lax.div(s, n)
        return d, pltpu.make_async_remote_copy(
            src_ref=src.at[s],
            dst_ref=dst.at[k, slot],
            send_sem=c_send.at[which, s],
            recv_sem=c_recv.at[which, k, slot],
            device_id={"kv": d},
        )

    def shard(s, carry):
        d = owner_of(s)

        @pl.when(d != me)
        def _():
            pltpu.make_async_remote_copy(
                src_ref=qbuf.at[s],
                dst_ref=qbuf.at[s],
                send_sem=b_send.at[0, 0],
                recv_sem=b_recv.at[s],
                device_id={"kv": d},
            ).wait_recv()

        pltpu.make_async_copy(keys_hbm.at[s], keys.at[s], cache_sem.at[0, s]).wait()
        pltpu.make_async_copy(values_hbm.at[s], values.at[s], cache_sem.at[1, s]).wait()
        q = spread(unfold(qbuf[s]))
        fade = decay[s]
        fade = jnp.concatenate(
            [jnp.broadcast_to(fade[h : h + 1], (props, pos_dev)) for h in range(heads)], axis=0
        )
        scores = dot_nt(q, keys[s]) * scale + fade
        live = position < lengths[s]
        scores = jnp.where(live, scores, LOW)
        top = jnp.max(scores, axis=1, keepdims=True)
        w = jnp.where(live, jnp.exp(scores - top), 0.0)
        total = jnp.sum(w, axis=1, keepdims=True)
        mix[s] = fold(gather_diag(dot(w.astype(BF16), values[s]))).astype(BF16)
        stat[s] = to_lanes(top, 0) + to_lanes(total, heads)
        for which, (src, dst) in enumerate(((mix, mix_in), (stat, stat_in))):
            _, copy = c_copy(s, which, src, dst)
            pl.when(d != me)(copy.start)
        return carry

    lax.fori_loop(0, seqs, shard, 0)

    ex_r = lax.broadcasted_iota(jnp.int32, (LANES, width), 0)
    ex_c = lax.broadcasted_iota(jnp.int32, (LANES, width), 1)
    widen = (ex_r == lax.div(ex_c, head_dim)).astype(F32)

    def merge(r):
        s = slot_seq(r)
        for k in range(1, n):
            for which, (src, dst) in enumerate(((mix, mix_in), (stat, stat_in))):
                pltpu.make_async_remote_copy(
                    src_ref=src.at[0],
                    dst_ref=dst.at[k - 1, r],
                    send_sem=c_send.at[which, 0],
                    recv_sem=c_recv.at[which, k - 1, r],
                    device_id={"kv": lax.rem(me + k, n)},
                ).wait_recv()
        stats = jnp.concatenate([stat[s]] + [stat_in[k, r] for k in range(n - 1)], axis=0)
        totals = pltpu.roll(stats, LANES - heads, 1).reshape(n, props, LANES)
        tops = stats.reshape(n, props, LANES) + path_s[r][None]
        tops = jnp.where((lane_p < heads)[None], tops, LOW)
        ttop = jnp.where(lane_p < heads, tstat[r, 0], LOW)
        best = jnp.maximum(jnp.max(tops, axis=0), ttop)
        factors = jnp.exp(tops - best[None])
        tfactor = jnp.exp(ttop - best)
        denom = jnp.sum(factors * totals, axis=0) + tfactor * tstat[r, 1]
        packed = jnp.concatenate([factors.reshape(n * props, LANES), tfactor, denom], axis=0)
        wide = dot(packed, widen, HIGH)
        numer = wide[n * props : (n + 1) * props] * tmix[r] + wide[:props] * unfold(mix[s])
        for k in range(1, n):
            numer = numer + wide[k * props : (k + 1) * props] * unfold(mix_in[k - 1, r])
        att[s] = fold(numer / wide[(n + 1) * props :]).astype(BF16)
        for k in range(1, n):
            b_copy(r, k, att, d_send, d_recv).start()

    for r in range(slots):
        for_slot(r, functools.partial(merge, r))

    for s in range(seqs):
        d = owner_of(s)

        @pl.when(d != me)
        def _(s=s, d=d):
            pltpu.make_async_remote_copy(
                src_ref=att.at[s],
                dst_ref=att.at[s],
                send_sem=d_send.at[0, 0],
                recv_sem=d_recv.at[s],
                device_id={"kv": d},
            ).wait_recv()

    out_load.wait()
    attended = jnp.concatenate([unfold(att[s]) for s in range(seqs)], axis=0).astype(BF16)
    block = rows // n_tp
    term = dot(attended, out_w[...])
    for t in range(n_tp):
        terms[t] = term[t * block : (t + 1) * block].astype(BF16)

    def e_copy(k):
        t = lax.rem(tp + k, n_tp)
        return pltpu.make_async_remote_copy(
            src_ref=terms.at[t],
            dst_ref=terms_in.at[n_tp - k - 1],
            send_sem=e_send.at[k - 1],
            recv_sem=e_recv.at[n_tp - k - 1],
            device_id={"tp": t},
        )

    for k in range(1, n_tp):
        e_copy(k).start()
    total = terms[tp].astype(F32)
    for k in range(1, n_tp):
        e_copy(n_tp - k).wait_recv()
        total = total + terms_in[k - 1].astype(F32)
    out[...] = total.astype(BF16)

    for s in range(seqs):
        d, copy = a_copy(s)
        pl.when(d != me)(copy.wait_send)
        for which, (src, dst) in enumerate(((mix, mix_in), (stat, stat_in))):
            _, copy = c_copy(s, which, src, dst)
            pl.when(d != me)(copy.wait_send)
    for r in range(slots):

        def drain(r=r):
            for k in range(1, n):
                b_copy(r, k, qbuf, b_send, b_recv).wait_send()
                b_copy(r, k, att, d_send, d_recv).wait_send()

        for_slot(r, drain)
    for k in range(1, n_tp):
        e_copy(k).wait_send()


def solution(mesh):
    n, n_tp = mesh.shape["kv"], mesh.shape["tp"]

    def body(
        tokens,
        norm_gain,
        query_weight,
        key_weight,
        value_weight,
        gate_weight,
        gate_bias,
        out_weight,
        cache_keys,
        cache_values,
        cache_decay,
        lengths,
        parents,
    ):
        rows, depth = tokens.shape
        seqs, props = parents.shape
        heads = cache_decay.shape[1]
        pos_dev = cache_keys.shape[1]
        width = query_weight.shape[1]
        cols = out_weight.shape[1]
        slots = -(-seqs // n)
        block = rows // n_tp
        all_w = 3 * width + LANES
        folded = (2 * props, width // 2)
        vmem = pl.BlockSpec(memory_space=pltpu.VMEM)
        hbm = pl.BlockSpec(memory_space=pl.ANY)
        smem = pl.BlockSpec(memory_space=pltpu.SMEM)
        dma = pltpu.SemaphoreType.DMA
        return pl.pallas_call(
            functools.partial(kernel, n, n_tp),
            out_shape=jax.ShapeDtypeStruct((block, cols), BF16),
            in_specs=[vmem, vmem, vmem, vmem, vmem, hbm, vmem, hbm, hbm, hbm, vmem, smem, vmem],
            out_specs=vmem,
            scratch_shapes=[
                pltpu.VMEM((seqs, props, all_w), F32),
                pltpu.VMEM((n - 1, slots, props, all_w), F32),
                pltpu.VMEM((depth, gate_weight.shape[1]), BF16),
                pltpu.VMEM(out_weight.shape, BF16),
                pltpu.VMEM(cache_keys.shape, BF16),
                pltpu.VMEM(cache_values.shape, BF16),
                pltpu.VMEM((seqs,) + folded, BF16),
                pltpu.VMEM((seqs,) + folded, BF16),
                pltpu.VMEM((seqs, props, LANES), F32),
                pltpu.VMEM((n - 1, slots) + folded, BF16),
                pltpu.VMEM((n - 1, slots, props, LANES), F32),
                pltpu.VMEM((seqs,) + folded, BF16),
                pltpu.VMEM((slots, props, LANES), F32),
                pltpu.VMEM((slots, props, LANES), F32),
                pltpu.VMEM((slots, props, width), F32),
                pltpu.VMEM((slots, 2, props, LANES), F32),
                pltpu.VMEM((slots, 2, LANES, width), F32),
                pltpu.VMEM((n_tp, block, cols), BF16),
                pltpu.VMEM((n_tp - 1, block, cols), BF16),
                pltpu.VMEM((-(-seqs // 8) * 8, LANES), jnp.int32),
                dma((2,)),
                dma((2, seqs)),
                dma((seqs,)),
                dma((n - 1, slots)),
                dma((slots, n - 1)),
                dma((seqs,)),
                dma((2, seqs)),
                dma((2, n - 1, slots)),
                dma((slots, n - 1)),
                dma((seqs,)),
                dma((n_tp - 1,)),
                dma((n_tp - 1,)),
            ],
            compiler_params=pltpu.CompilerParams(
                collective_id=0, has_side_effects=True, vmem_limit_bytes=48 * 1024 * 1024
            ),
        )(
            tokens,
            norm_gain.reshape(1, depth),
            query_weight,
            key_weight,
            value_weight,
            gate_weight,
            gate_bias.reshape(1, gate_bias.shape[0]),
            out_weight,
            cache_keys,
            cache_values,
            cache_decay,
            lengths,
            parents,
        )

    in_specs = (
        P(None, "kv"),
        P("kv"),
        P("kv", "tp"),
        P("kv", "tp"),
        P("kv", "tp"),
        P(),
        P(),
        P("tp", "kv"),
        P(None, "kv", "tp"),
        P(None, "kv", "tp"),
        P(None, "tp", "kv"),
        P(),
        P(),
    )
    out_specs = P("tp", "kv")
    return jax.shard_map(body, mesh=mesh, in_specs=in_specs, out_specs=out_specs, check_vma=False)
```

```python
import functools

import jax
import jax.numpy as jnp
from jax import lax
from jax.experimental import pallas as pl
from jax.experimental.pallas import tpu as pltpu
from jax.sharding import PartitionSpec as P

F32 = jnp.float32
BF16 = jnp.bfloat16
LANES = 128
LOW = -1e30
NT = (((1,), (1,)), ((), ()))
HIGH = lax.Precision.HIGHEST


def dot(a, b, precision=None):
    return jnp.dot(a, b, preferred_element_type=F32, precision=precision)


def dot_nt(a, b, precision=None):
    return lax.dot_general(a, b, NT, preferred_element_type=F32, precision=precision)


def fold(x):
    half = x.shape[1] // 2
    return jnp.concatenate([x[:, :half], x[:, half:]], axis=0)


def unfold(x):
    rows = x.shape[0] // 2
    x = x.astype(F32)
    return jnp.concatenate([x[:rows], x[rows:]], axis=1)


def kernel(
    n,
    n_tp,
    tokens,
    gain,
    query_w,
    key_w,
    value_w,
    gate_hbm,
    bias,
    out_hbm,
    keys_hbm,
    values_hbm,
    decay,
    lengths,
    parents,
    out,
    part,
    part_v,
    pair_in,
    pair_in_v,
    part_in,
    part_in_v,
    gate_w,
    out_w,
    keys,
    values,
    qbuf,
    mix,
    stat,
    mix_in,
    stat_in,
    att,
    anc,
    path_s,
    tmix,
    tstat,
    kvnew,
    terms,
    terms_in,
    par_pad,
    load_sem,
    cache_sem,
    p_send,
    p_recv,
    a_send,
    a_recv,
    b_send,
    b_recv,
    c_send,
    c_recv,
    d_send,
    d_recv,
    e_send,
    e_recv,
):
    me = lax.axis_index("kv")
    tp = lax.axis_index("tp")
    rows, depth = tokens.shape
    seqs, props = parents.shape
    heads = decay.shape[1]
    pos_dev = keys.shape[1]
    width = query_w.shape[1]
    head_dim = width // heads
    scale = head_dim ** (-0.5)
    slots = part_in.shape[1]
    parity = lax.rem(tp, 2)
    left_over = seqs % n
    hp = heads * props

    barrier = pltpu.get_barrier_semaphore()
    for k in range(1, n):
        pl.semaphore_signal(barrier, inc=1, device_id={"kv": lax.rem(me + k, n)})
    for k in range(1, n_tp):
        pl.semaphore_signal(barrier, inc=1, device_id={"tp": lax.rem(tp + k, n_tp)})

    gate_load = pltpu.make_async_copy(
        gate_hbm.at[pl.ds(pl.multiple_of(me * depth, depth), depth), :], gate_w, load_sem.at[0]
    )
    gate_load.start()
    cache_loads = []
    for s in range(seqs):
        k_load = pltpu.make_async_copy(keys_hbm.at[s], keys.at[s], cache_sem.at[0, s])
        v_load = pltpu.make_async_copy(values_hbm.at[s], values.at[s], cache_sem.at[1, s])
        k_load.start()
        v_load.start()
        cache_loads.append((k_load, v_load))
    out_load = pltpu.make_async_copy(out_hbm, out_w, load_sem.at[1])
    out_load.start()

    def owner_of(s):
        if isinstance(s, int):
            place = s % n
            shift = parity * left_over if s // n == seqs // n else 0
        else:
            place = lax.rem(s, n)
            shift = jnp.where(lax.div(s, n) == seqs // n, parity * left_over, 0)
        return lax.rem(place + shift, n)

    def slot_seq(r):
        shift = parity * left_over if r == seqs // n else 0
        return r * n + lax.rem(me + 2 * n - shift, n)

    def for_slot(r, f):
        if (r + 1) * n <= seqs:
            f()
        else:
            pl.when(slot_seq(r) < seqs)(f)

    xf = tokens[...].astype(F32)
    squares = jnp.sum(xf * xf, axis=1, keepdims=True)
    normed = (xf * gain[...]).astype(BF16)
    sel_rows = lax.broadcasted_iota(jnp.int32, (bias.shape[1], LANES), 0)
    sel_cols = lax.broadcasted_iota(jnp.int32, (bias.shape[1], LANES), 1)
    select = ((sel_rows == sel_cols + tp * heads) & (sel_cols < heads)).astype(F32)
    for i, w in enumerate((query_w, key_w)):
        part[:, :, i * width : (i + 1) * width] = dot(normed, w[...]).reshape(seqs, props, width)
    value_part = dot(normed, value_w[...])
    for s in range(seqs):
        part_v[s] = fold(value_part[s * props : (s + 1) * props]).astype(BF16)
    gate_load.wait()
    gates_w = dot(gate_w[...], select.astype(BF16)).astype(BF16)
    gate_part = dot(normed, gates_w)
    lane = lax.broadcasted_iota(jnp.int32, (rows, LANES), 1)
    gate_part = jnp.where(lane == LANES // 2, squares, gate_part)
    part[:, :, 2 * width :] = gate_part.reshape(seqs, props, LANES)
    pl.semaphore_wait(barrier, n + n_tp - 2)

    side = lax.rem(me, 2)
    partner = me + 1 - 2 * side
    n_far = n // 2
    shares = ((part, pair_in, part_in), (part_v, pair_in_v, part_in_v))

    def p_copy(s, which):
        src, dst, _ = shares[which]
        return pltpu.make_async_remote_copy(
            src_ref=src.at[s],
            dst_ref=dst.at[s],
            send_sem=p_send.at[which, s],
            recv_sem=p_recv.at[which, s],
            device_id={"kv": partner},
        )

    def a_copy(s, which):
        src, _, dst = shares[which]
        d = owner_of(s)
        k = jnp.maximum(lax.rem(lax.div(me, 2) - lax.div(d, 2) + n_far, n_far) - 1, 0)
        return pltpu.make_async_remote_copy(
            src_ref=src.at[s],
            dst_ref=dst.at[k, s // n],
            send_sem=a_send.at[which, s],
            recv_sem=a_recv.at[which, k, s // n],
            device_id={"kv": d},
        )

    def crosses(s):
        return lax.rem(owner_of(s), 2) != side

    def passes(s):
        d = owner_of(s)
        return (lax.rem(d, 2) == side) & (d != me)

    for s in range(seqs):
        for which in range(2):
            pl.when(crosses(s))(p_copy(s, which).start)

    par_pad[...] = jnp.zeros(par_pad.shape, jnp.int32)
    par_pad[0:seqs, 0:props] = parents[...]
    r_i = lax.broadcasted_iota(jnp.int32, (LANES, LANES), 0)
    c_i = lax.broadcasted_iota(jnp.int32, (LANES, LANES), 1)
    eye = (r_i == c_i).astype(F32)
    bias_row = dot(jnp.broadcast_to(bias[...], (8, bias.shape[1])), select, HIGH)[0:1]

    def ancestry(r):
        s = slot_seq(r)
        row = par_pad[pl.ds(s, 1), :]
        link = jnp.maximum((row == r_i).astype(F32), eye).astype(BF16)
        for _ in range(props.bit_length()):
            link = jnp.minimum(dot(link, link), 1.0).astype(BF16)
        anc[r] = dot_nt(eye.astype(BF16), link)[:props]

    for r in range(slots):
        for_slot(r, functools.partial(ancestry, r))

    def pass_on(s):
        for which in range(2):
            p_copy(s, which).wait_recv()
        part[s] = part[s] + pair_in[s]
        part_v[s] = (part_v[s].astype(F32) + pair_in_v[s].astype(F32)).astype(BF16)
        for which in range(2):
            a_copy(s, which).start()

    for s in range(seqs):
        pl.when(passes(s))(functools.partial(pass_on, s))

    lane_p = lax.broadcasted_iota(jnp.int32, (props, LANES), 1)
    bd_row = lax.broadcasted_iota(jnp.int32, (heads, props, width), 0)
    bd_col = lax.broadcasted_iota(jnp.int32, (heads, props, width), 2)
    diag = (lax.div(bd_col, head_dim) == bd_row).reshape(hp, width)

    def spread(q):
        wide = jnp.broadcast_to(q[None], (heads, props, width)).reshape(hp, width)
        return jnp.where(diag, wide, 0.0).astype(BF16)

    def gather_diag(m):
        return jnp.sum(jnp.where(diag, m, 0.0).reshape(heads, props, width), axis=0)

    def to_lanes(col, first):
        acc = jnp.zeros((props, LANES), F32)
        for h in range(heads):
            acc = jnp.where(lane_p == h + first, col[h * props : (h + 1) * props], acc)
        return acc

    def b_copy(r, k, buf, send, recv):
        s = slot_seq(r)
        return pltpu.make_async_remote_copy(
            src_ref=buf.at[s],
            dst_ref=buf.at[s],
            send_sem=send.at[r, k - 1],
            recv_sem=recv.at[s],
            device_id={"kv": lax.rem(me + k, n)},
        )

    pad_rows = LANES - props

    def project(r):
        s = slot_seq(r)
        for which, (src, near, far) in enumerate(shares):
            pltpu.make_async_remote_copy(
                src_ref=src.at[0],
                dst_ref=near.at[s],
                send_sem=p_send.at[which, 0],
                recv_sem=p_recv.at[which, s],
                device_id={"kv": partner},
            ).wait_recv()
            for k in range(1, n_far):
                pltpu.make_async_remote_copy(
                    src_ref=src.at[0],
                    dst_ref=far.at[k - 1, r],
                    send_sem=a_send.at[which, 0],
                    recv_sem=a_recv.at[which, k - 1, r],
                    device_id={"kv": lax.rem(me + 2 * k, n)},
                ).wait_recv()
        total = part[s] + pair_in[s]
        total_v = unfold(part_v[s]) + unfold(pair_in_v[s])
        for k in range(1, n_far):
            total = total + part_in[k - 1, r]
            total_v = total_v + unfold(part_in_v[k - 1, r])
        tail = total[:, 2 * width :]
        square = jnp.sum(jnp.where(lane_p == LANES // 2, tail, 0.0), axis=1, keepdims=True)
        inverse = lax.rsqrt(square / (depth * n) + 1e-06)
        q = inverse * total[:, :width]
        qbuf[s] = fold(q).astype(BF16)
        for k in range(1, n):
            b_copy(r, k, qbuf, b_send, b_recv).start()
        kvnew[r, 0, 0:props] = inverse * total[:, width : 2 * width]
        kvnew[r, 1, 0:props] = inverse * total_v
        kvnew[r, :, props:] = jnp.zeros((2, pad_rows, width), F32)
        x = inverse * tail + bias_row
        log_gate = jnp.minimum(x, 0.0) - jnp.log1p(jnp.exp(-jnp.abs(x)))
        padded = jnp.concatenate([log_gate, jnp.zeros((pad_rows, LANES), F32)], axis=0)
        path_s[r] = dot(anc[r], padded, HIGH)

    def tree(r):
        s = slot_seq(r)
        path = path_s[r]
        q = spread(unfold(qbuf[s]))
        head_of = lax.broadcasted_iota(jnp.int32, (heads, props, LANES), 0)
        lane_of = lax.broadcasted_iota(jnp.int32, (heads, props, LANES), 2)
        pick = (head_of == lane_of).reshape(hp, LANES)
        tiled = jnp.broadcast_to(path[None], (heads, props, LANES)).reshape(hp, LANES)
        own = jnp.sum(jnp.where(pick, tiled, 0.0), axis=1, keepdims=True)
        padded = jnp.concatenate([path, jnp.zeros((pad_rows, LANES), F32)], axis=0)
        other = dot_nt(pick.astype(F32), padded, HIGH)
        scores = dot_nt(q, kvnew[r, 0].astype(BF16)) * scale + own - other
        live = jnp.broadcast_to(anc[r][None], (heads, props, LANES)).reshape(hp, LANES) > 0.5
        scores = jnp.where(live, scores, LOW)
        top = jnp.max(scores, axis=1, keepdims=True)
        w = jnp.where(live, jnp.exp(scores - top), 0.0)
        total = jnp.sum(w, axis=1, keepdims=True)
        tmix[r] = gather_diag(dot(w.astype(BF16), kvnew[r, 1].astype(BF16)))
        tstat[r, 0] = to_lanes(top, 0)
        tstat[r, 1] = to_lanes(total, 0)

    position = lax.broadcasted_iota(jnp.int32, (hp, pos_dev), 1) + me * pos_dev

    def c_copy(s, which, src, dst):
        d = owner_of(s)
        k = jnp.maximum(lax.rem(me - d + n, n) - 1, 0)
        slot = s // n if isinstance(s, int) else lax.div(s, n)
        return d, pltpu.make_async_remote_copy(
            src_ref=src.at[s],
            dst_ref=dst.at[k, slot],
            send_sem=c_send.at[which, s],
            recv_sem=c_recv.at[which, k, slot],
            device_id={"kv": d},
        )

    def shard(s, carry):
        d = owner_of(s)

        @pl.when(d != me)
        def _():
            pltpu.make_async_remote_copy(
                src_ref=qbuf.at[s],
                dst_ref=qbuf.at[s],
                send_sem=b_send.at[0, 0],
                recv_sem=b_recv.at[s],
                device_id={"kv": d},
            ).wait_recv()

        pltpu.make_async_copy(keys_hbm.at[s], keys.at[s], cache_sem.at[0, s]).wait()
        pltpu.make_async_copy(values_hbm.at[s], values.at[s], cache_sem.at[1, s]).wait()
        q = spread(unfold(qbuf[s]))
        fade = decay[s]
        fade = jnp.concatenate(
            [jnp.broadcast_to(fade[h : h + 1], (props, pos_dev)) for h in range(heads)], axis=0
        )
        scores = dot_nt(q, keys[s]) * scale + fade
        live = position < lengths[s]
        scores = jnp.where(live, scores, LOW)
        top = jnp.max(scores, axis=1, keepdims=True)
        w = jnp.where(live, jnp.exp(scores - top), 0.0)
        total = jnp.sum(w, axis=1, keepdims=True)
        mix[s] = fold(gather_diag(dot(w.astype(BF16), values[s]))).astype(BF16)
        stat[s] = to_lanes(top, 0) + to_lanes(total, heads)
        for which, (src, dst) in enumerate(((mix, mix_in), (stat, stat_in))):
            _, copy = c_copy(s, which, src, dst)
            pl.when(d != me)(copy.start)
        return carry

    ex_r = lax.broadcasted_iota(jnp.int32, (LANES, width), 0)
    ex_c = lax.broadcasted_iota(jnp.int32, (LANES, width), 1)
    widen = (ex_r == lax.div(ex_c, head_dim)).astype(F32)

    def merge(r):
        s = slot_seq(r)
        for k in range(1, n):
            for which, (src, dst) in enumerate(((mix, mix_in), (stat, stat_in))):
                pltpu.make_async_remote_copy(
                    src_ref=src.at[0],
                    dst_ref=dst.at[k - 1, r],
                    send_sem=c_send.at[which, 0],
                    recv_sem=c_recv.at[which, k - 1, r],
                    device_id={"kv": lax.rem(me + k, n)},
                ).wait_recv()
        stats = jnp.concatenate([stat[s]] + [stat_in[k, r] for k in range(n - 1)], axis=0)
        totals = pltpu.roll(stats, LANES - heads, 1).reshape(n, props, LANES)
        tops = stats.reshape(n, props, LANES) + path_s[r][None]
        tops = jnp.where((lane_p < heads)[None], tops, LOW)
        ttop = jnp.where(lane_p < heads, tstat[r, 0], LOW)
        best = jnp.maximum(jnp.max(tops, axis=0), ttop)
        factors = jnp.exp(tops - best[None])
        tfactor = jnp.exp(ttop - best)
        denom = jnp.sum(factors * totals, axis=0) + tfactor * tstat[r, 1]
        packed = jnp.concatenate([factors.reshape(n * props, LANES), tfactor, denom], axis=0)
        wide = dot(packed, widen, HIGH)
        numer = wide[n * props : (n + 1) * props] * tmix[r] + wide[:props] * unfold(mix[s])
        for k in range(1, n):
            numer = numer + wide[k * props : (k + 1) * props] * unfold(mix_in[k - 1, r])
        att[s] = fold(numer / wide[(n + 1) * props :]).astype(BF16)
        for k in range(1, n):
            b_copy(r, k, att, d_send, d_recv).start()

    for r in range(slots):
        for_slot(r, functools.partial(project, r))
        if r > 0:
            for_slot(r - 1, functools.partial(merge, r - 1))
        for_slot(r, functools.partial(tree, r))
        lax.fori_loop(r * n, min((r + 1) * n, seqs), shard, 0)
    for_slot(slots - 1, functools.partial(merge, slots - 1))

    out_load.wait()
    block = rows // n_tp

    def e_copy(t):
        k = lax.rem(tp - t + n_tp, n_tp)
        return pltpu.make_async_remote_copy(
            src_ref=terms.at[t],
            dst_ref=terms_in.at[jnp.maximum(k - 1, 0)],
            send_sem=e_send.at[t],
            recv_sem=e_recv.at[jnp.maximum(k - 1, 0)],
            device_id={"tp": t},
        )

    arrived = 0
    for t in range(n_tp):
        first, last = t * block // props, ((t + 1) * block - 1) // props + 1
        for s in range(arrived, last):
            d = owner_of(s)

            @pl.when(d != me)
            def _(s=s, d=d):
                pltpu.make_async_remote_copy(
                    src_ref=att.at[s],
                    dst_ref=att.at[s],
                    send_sem=d_send.at[0, 0],
                    recv_sem=d_recv.at[s],
                    device_id={"kv": d},
                ).wait_recv()

        arrived = max(arrived, last)
        attended = jnp.concatenate([unfold(att[s]) for s in range(first, last)], axis=0)
        term = dot(attended.astype(BF16), out_w[...])
        begin = t * block - first * props
        terms[t] = term[begin : begin + block].astype(BF16)
        pl.when(tp != t)(e_copy(t).start)
    total = terms[tp].astype(F32)
    for k in range(1, n_tp):
        pltpu.make_async_remote_copy(
            src_ref=terms.at[0],
            dst_ref=terms_in.at[k - 1],
            send_sem=e_send.at[0],
            recv_sem=e_recv.at[k - 1],
            device_id={"tp": lax.rem(tp + k, n_tp)},
        ).wait_recv()
        total = total + terms_in[k - 1].astype(F32)
    out[...] = total.astype(BF16)

    for s in range(seqs):
        d = owner_of(s)
        for which in range(2):
            pl.when(crosses(s))(p_copy(s, which).wait_send)
            pl.when(passes(s))(a_copy(s, which).wait_send)
        for which, (src, dst) in enumerate(((mix, mix_in), (stat, stat_in))):
            _, copy = c_copy(s, which, src, dst)
            pl.when(d != me)(copy.wait_send)
    for r in range(slots):

        def drain(r=r):
            for k in range(1, n):
                b_copy(r, k, qbuf, b_send, b_recv).wait_send()
                b_copy(r, k, att, d_send, d_recv).wait_send()

        for_slot(r, drain)
    for t in range(n_tp):
        pl.when(tp != t)(e_copy(t).wait_send)


def solution(mesh):
    n, n_tp = mesh.shape["kv"], mesh.shape["tp"]

    def body(
        tokens,
        norm_gain,
        query_weight,
        key_weight,
        value_weight,
        gate_weight,
        gate_bias,
        out_weight,
        cache_keys,
        cache_values,
        cache_decay,
        lengths,
        parents,
    ):
        rows, depth = tokens.shape
        seqs, props = parents.shape
        heads = cache_decay.shape[1]
        pos_dev = cache_keys.shape[1]
        width = query_weight.shape[1]
        cols = out_weight.shape[1]
        slots = -(-seqs // n)
        block = rows // n_tp
        all_w = 2 * width + LANES
        folded = (2 * props, width // 2)
        vmem = pl.BlockSpec(memory_space=pltpu.VMEM)
        hbm = pl.BlockSpec(memory_space=pl.ANY)
        smem = pl.BlockSpec(memory_space=pltpu.SMEM)
        dma = pltpu.SemaphoreType.DMA
        return pl.pallas_call(
            functools.partial(kernel, n, n_tp),
            out_shape=jax.ShapeDtypeStruct((block, cols), BF16),
            in_specs=[vmem, vmem, vmem, vmem, vmem, hbm, vmem, hbm, hbm, hbm, vmem, smem, vmem],
            out_specs=vmem,
            scratch_shapes=[
                pltpu.VMEM((seqs, props, all_w), F32),
                pltpu.VMEM((seqs,) + folded, BF16),
                pltpu.VMEM((seqs, props, all_w), F32),
                pltpu.VMEM((seqs,) + folded, BF16),
                pltpu.VMEM((n // 2 - 1, slots, props, all_w), F32),
                pltpu.VMEM((n // 2 - 1, slots) + folded, BF16),
                pltpu.VMEM((depth, gate_weight.shape[1]), BF16),
                pltpu.VMEM(out_weight.shape, BF16),
                pltpu.VMEM(cache_keys.shape, BF16),
                pltpu.VMEM(cache_values.shape, BF16),
                pltpu.VMEM((seqs,) + folded, BF16),
                pltpu.VMEM((seqs,) + folded, BF16),
                pltpu.VMEM((seqs, props, LANES), F32),
                pltpu.VMEM((n - 1, slots) + folded, BF16),
                pltpu.VMEM((n - 1, slots, props, LANES), F32),
                pltpu.VMEM((seqs,) + folded, BF16),
                pltpu.VMEM((slots, props, LANES), F32),
                pltpu.VMEM((slots, props, LANES), F32),
                pltpu.VMEM((slots, props, width), F32),
                pltpu.VMEM((slots, 2, props, LANES), F32),
                pltpu.VMEM((slots, 2, LANES, width), F32),
                pltpu.VMEM((n_tp, block, cols), BF16),
                pltpu.VMEM((n_tp - 1, block, cols), BF16),
                pltpu.VMEM((-(-seqs // 8) * 8, LANES), jnp.int32),
                dma((2,)),
                dma((2, seqs)),
                dma((2, seqs)),
                dma((2, seqs)),
                dma((2, seqs)),
                dma((2, n // 2 - 1, slots)),
                dma((slots, n - 1)),
                dma((seqs,)),
                dma((2, seqs)),
                dma((2, n - 1, slots)),
                dma((slots, n - 1)),
                dma((seqs,)),
                dma((n_tp,)),
                dma((n_tp - 1,)),
            ],
            compiler_params=pltpu.CompilerParams(
                collective_id=0, has_side_effects=True, vmem_limit_bytes=48 * 1024 * 1024
            ),
        )(
            tokens,
            norm_gain.reshape(1, depth),
            query_weight,
            key_weight,
            value_weight,
            gate_weight,
            gate_bias.reshape(1, gate_bias.shape[0]),
            out_weight,
            cache_keys,
            cache_values,
            cache_decay,
            lengths,
            parents,
        )

    in_specs = (
        P(None, "kv"),
        P("kv"),
        P("kv", "tp"),
        P("kv", "tp"),
        P("kv", "tp"),
        P(),
        P(),
        P("tp", "kv"),
        P(None, "kv", "tp"),
        P(None, "kv", "tp"),
        P(None, "tp", "kv"),
        P(),
        P(),
    )
    out_specs = P("tp", "kv")
    return jax.shard_map(body, mesh=mesh, in_specs=in_specs, out_specs=out_specs, check_vma=False)
```
